32 devices in a mesh: sp: 16 (over z, y, core), tp: 2 (over x).
Axes of the slice: x: 2, y: 2, z: 4, core: 2. Of those that a mesh axis runs over, the one named last changes fastest.
Arguments:
- residual: bfloat16 [2048, 2048], P(('sp', 'tp')), may hold values from -6 to 6
- forget_forward: bfloat16 [2048, 1024], P('sp', 'tp'), may hold values from -5.5 to 5.5
- forget_backward: bfloat16 [2048, 1024], P('sp', 'tp'), may hold values from -5.5 to 5.5
- value_written: bfloat16 [2048, 1024], P('sp', 'tp'), may hold values from -6 to 6
- query_logits: bfloat16 [2048, 1024], P('sp', 'tp'), may hold values from -6 to 6
- output_gate_logits: bfloat16 [2048, 1024], P('sp', 'tp'), may hold values from -6 to 6
- forget_minimum: float32 [2, 1024], P(None, 'tp'), may hold values from 0.88 to 1
- extra_log_rate: float32 [2, 2048, 8], P(None, 'sp', 'tp'), may hold values from -0.7 to 0
- head_norm_scale: float32 [128], replicated, may hold values from 0.1 to 1.9
- output_matrix: bfloat16 [1024, 2048], P(None, 'sp'), may hold values from -0.1875 to 0.1875
- prenorm_scale: float32 [2048], replicated, may hold values from 0.1 to 1.9
- gate_up_matrix: bfloat16 [2048, 5632], P('sp', 'tp'), may hold values from -0.125 to 0.125
- value_up_matrix: bfloat16 [2048, 5632], P('sp', 'tp'), may hold values from -0.125 to 0.125
- gate_taps: float32 [3, 5632], P(None, 'tp'), may hold values from -3.5 to 3.5
- value_taps: float32 [3, 5632], P(None, 'tp'), may hold values from -3.5 to 3.5
- down_matrix: bfloat16 [5632, 2048], P('tp', 'sp'), may hold values from -0.078125 to 0.078125
Outputs:
- layer_out: bfloat16 [2048, 2048], P(('sp', 'tp'))
The draws below stay inside these ranges and needn't reach their ends.
All inputs are finite; a program needn't handle non-finite values.
Results may differ from the reference program's by a relative error of at most 0.012.
Values may be sent and summed in bfloat16 or wider, within the bound.
No kernel may reach another device: no remote copies, remote signals or barrier semaphores. Data moves between devices by JAX's collectives and lax.ppermute only.
A program may use at most 128 MiB of HBM per device.

```python
import jax
import jax.numpy as jnp
from jax import lax

D = 2048
HEADS = 8
HEAD_WIDTH = 128
HW = 1024
FF = 5632
BLOCK = 64
TOK_DEV = 128
TOKENS = 2048
N_TP = 2


def forget_draw(key):
    noise = jnp.clip(jax.random.normal(jax.random.fold_in(key, 1), (TOKENS, HEADS * HEAD_WIDTH), jnp.float32), -4.0, 4.0)
    shifts = jax.random.uniform(jax.random.fold_in(key, 2), (TOKENS // TOK_DEV, 1, 1), jnp.float32, -1.5, 1.5)
    noise = (noise.reshape(TOKENS // TOK_DEV, TOK_DEV, HEADS * HEAD_WIDTH) + shifts).reshape(TOKENS, HEADS * HEAD_WIDTH)
    return noise.astype(jnp.bfloat16)


def draw_forget_forward(key, part):
    return forget_draw(jax.random.fold_in(key, 11))


def draw_forget_backward(key, part):
    return forget_draw(jax.random.fold_in(key, 12))


def draw_forget_minimum(key, part):
    fast_count = 4
    picks = jax.random.randint(jax.random.fold_in(key, 21), (2, HEADS, 1), 0, 8)
    fast_bound = jax.random.uniform(jax.random.fold_in(key, 22), (2, HEADS, HEAD_WIDTH), jnp.float32, 0.88, 0.92)
    slow_bound = 1.0 - jax.random.uniform(jax.random.fold_in(key, 23), (2, HEADS, HEAD_WIDTH), jnp.float32, 0.5, 1.5) / TOKENS
    forget_floor = jnp.where(picks < fast_count, fast_bound, slow_bound)
    return forget_floor.reshape(2, HEADS * HEAD_WIDTH).astype(jnp.float32)


def draw_extra_log_rate(key, part):
    spots = jax.random.randint(jax.random.fold_in(key, 31), (2, 1, 3), 0, TOKENS)
    places = jnp.arange(TOKENS, dtype=jnp.int32)[None, :, None]
    struck = jnp.any(places == spots, axis=-1)[:, :, None]
    depth = jnp.log(jax.random.uniform(jax.random.fold_in(key, 32), (2, TOKENS, HEADS), jnp.float32, 0.5, 0.8))
    return jnp.where(struck, depth, 0.0).astype(jnp.float32)


def block_levels(own_key, shape, cuts, least, top_value):
    gain = 1.0
    for dim, parts in cuts:
        heights = jax.random.uniform(jax.random.fold_in(jax.random.fold_in(own_key, 6), dim), (parts,), jnp.float32, least / len(cuts), top_value / len(cuts))
        gain = gain * jnp.repeat(jnp.exp(heights), shape[dim] // parts).reshape((-1,) + (1,) * (len(shape) - 1 - dim))
    return gain


def normal_values(rng, extent, scale, bound, cuts=(), kind=jnp.bfloat16):
    result = scale * jax.random.normal(rng, extent, jnp.float32)
    if cuts:
        result = result * block_levels(rng, extent, cuts, -0.22, 0.18)
    return jnp.clip(result, -bound, bound).astype(kind)


def setup_inputs(seed: int = 0) -> dict:
    seeds = jax.random.split(jax.random.key(seed), 17)
    residual = normal_values(seeds[0], (TOKENS, D), 1.0, 6.0, ((0, 32),))
    forget_forward = draw_forget_forward(jax.random.fold_in(seeds[16], 71), 0)
    forget_backward = draw_forget_backward(jax.random.fold_in(seeds[16], 71), 0)
    value_written = normal_values(seeds[3], (TOKENS, HW), 1.0, 6.0, ((0, 16), (1, 2)))
    query_logits = normal_values(seeds[4], (TOKENS, HW), 1.0, 6.0, ((0, 16), (1, 2)))
    output_gate_logits = normal_values(seeds[5], (TOKENS, HW), 1.0, 6.0, ((0, 16), (1, 2)))
    forget_minimum = draw_forget_minimum(jax.random.fold_in(seeds[16], 71), 0)
    extra_log_rate = draw_extra_log_rate(jax.random.fold_in(seeds[16], 71), 0)
    head_norm_scale = jnp.clip(1.0 + 0.18 * jax.random.normal(seeds[8], (HEAD_WIDTH,), jnp.float32), 0.1, 1.9)
    output_matrix = normal_values(seeds[9], (HW, D), HW ** -0.5, 0.1875, ((1, 16),))
    prenorm_scale = jnp.clip(1.0 + 0.18 * jax.random.normal(seeds[10], (D,), jnp.float32), 0.1, 1.9)
    gate_up_matrix = normal_values(seeds[11], (D, FF), D ** -0.5, 0.125, ((0, 16), (1, 2)))
    value_up_matrix = normal_values(seeds[12], (D, FF), D ** -0.5, 0.125, ((0, 16), (1, 2)))
    gate_taps = normal_values(seeds[13], (3, FF), 3 ** -0.5, 3.5, ((1, 2),), jnp.float32)
    value_taps = normal_values(seeds[14], (3, FF), 3 ** -0.5, 3.5, ((1, 2),), jnp.float32)
    down_matrix = normal_values(seeds[15], (FF, D), FF ** -0.5, 0.078125, ((0, 2), (1, 16)))
    return dict(residual=residual, forget_forward=forget_forward, forget_backward=forget_backward, value_written=value_written, query_logits=query_logits, output_gate_logits=output_gate_logits, forget_minimum=forget_minimum, extra_log_rate=extra_log_rate, head_norm_scale=head_norm_scale, output_matrix=output_matrix, prenorm_scale=prenorm_scale, gate_up_matrix=gate_up_matrix, value_up_matrix=value_up_matrix, gate_taps=gate_taps, value_taps=value_taps, down_matrix=down_matrix)


EPSILON = 1e-06

def rms_scale(array):
    return array * lax.rsqrt(lax.optimization_barrier(jnp.mean(array * array, axis=-1, keepdims=True)) + EPSILON)

def forget_factors(forget_logits, forget_floor, extra_decay):
    unbounded_gate = forget_logits.astype(jnp.float32)
    log_forget_gate = jnp.log(forget_floor + (1.0 - forget_floor) * jax.nn.sigmoid(unbounded_gate)) + jnp.repeat(extra_decay, HEAD_WIDTH, axis=1)
    key_in = (1.0 - forget_floor) * jax.nn.sigmoid(-unbounded_gate)
    shape = (unbounded_gate.shape[0], unbounded_gate.shape[1] // HEAD_WIDTH, HEAD_WIDTH)
    return (log_forget_gate.reshape(shape), key_in.reshape(shape))

def block_scan(log_forget_gate, key_in, values, queries):
    length, heads, depth = log_forget_gate.shape
    width = values.shape[2]
    blocks = length // BLOCK
    highest = lax.Precision.HIGHEST
    lower = jnp.tril(jnp.ones((BLOCK, BLOCK), dtype=bool))[:, :, None, None]

    def split(array):
        return array.reshape(blocks, BLOCK, heads, array.shape[2])

    def advance(carry, pieces):
        state, carried = carry
        log_part, key_part, value_part, query_part = pieces
        running = jnp.cumsum(log_part, axis=0)
        block_total = running[-1]
        query_carry = query_part * jnp.exp(carried[None] + running)
        from_state = jnp.einsum('chd,hde->che', query_part * jnp.exp(running), state, precision=highest)
        gaps = jnp.where(lower, running[:, None] - running[None, :], -1e+30)
        scores = jnp.einsum('ihd,jhd,ijhd->hij', query_part, key_part, jnp.exp(gaps), precision=highest)
        inside = jnp.einsum('hij,jhe->ihe', scores, value_part, precision=highest)
        fresh = jnp.einsum('chd,che->hde', key_part * jnp.exp(block_total[None] - running), value_part, precision=highest)
        state = jnp.exp(block_total)[:, :, None] * state + fresh
        return ((state, carried + block_total), (from_state + inside, query_carry))
    start = (jnp.zeros((heads, depth, width), jnp.float32), jnp.zeros((heads, depth), jnp.float32))
    (state, carried), (outputs, query_carry) = lax.scan(advance, start, (split(log_forget_gate), split(key_in), split(values), split(queries)))
    return (state, carried, outputs.reshape(length, heads, width), query_carry.reshape(length, heads, depth))

def reference(residual, forget_forward, forget_backward, value_written, query_logits, output_gate_logits, forget_minimum, extra_log_rate, head_norm_scale, output_matrix, prenorm_scale, gate_up_matrix, value_up_matrix, gate_taps, value_taps, down_matrix):
    length = value_written.shape[0]
    shape = (length, value_written.shape[1] // HEAD_WIDTH, HEAD_WIDTH)
    values = value_written.astype(jnp.float32).reshape(shape)
    queries = jax.nn.silu(query_logits.astype(jnp.float32)).reshape(shape)
    log_decay_forward, key_forward = forget_factors(forget_forward, forget_minimum[0], extra_log_rate[0])
    forward = block_scan(log_decay_forward, key_forward, values, queries)[2]
    log_decay_backward, key_backward = forget_factors(forget_backward, forget_minimum[1], extra_log_rate[1])
    backward = block_scan(log_decay_backward[::-1], key_backward[::-1], values[::-1], queries[::-1])[2][::-1]
    gated = rms_scale(forward + backward) * head_norm_scale * jax.nn.silu(output_gate_logits.astype(jnp.float32)).reshape(shape)
    mixed_in = gated.reshape(length, shape[1] * HEAD_WIDTH).astype(jnp.bfloat16)
    after_mix = residual.astype(jnp.float32) + jnp.dot(mixed_in, output_matrix, preferred_element_type=jnp.float32)
    normed = (rms_scale(after_mix) * prenorm_scale).astype(jnp.bfloat16)
    gate_up = jnp.dot(normed, gate_up_matrix, preferred_element_type=jnp.float32).astype(jnp.bfloat16)
    value_up = jnp.dot(normed, value_up_matrix, preferred_element_type=jnp.float32).astype(jnp.bfloat16)

    def convolve(upward, kernel):
        padded = jnp.pad(upward, ((1, 1), (0, 0)))
        return padded[:length] * kernel[0] + padded[1:length + 1] * kernel[1] + padded[2:] * kernel[2]
    hidden = (jax.nn.silu(convolve(gate_up, gate_taps)) * convolve(value_up, value_taps)).astype(jnp.bfloat16)
    group_width = hidden.shape[1] // N_TP

    def add_group(index, total):
        first = (index * group_width).astype(jnp.int32)
        hidden_part = lax.dynamic_slice_in_dim(hidden, first, group_width, 1)
        weight_part = lax.dynamic_slice_in_dim(down_matrix, first, group_width, 0)
        partial_sum = jnp.dot(hidden_part, weight_part, preferred_element_type=jnp.float32)
        return total + lax.optimization_barrier(partial_sum.astype(jnp.bfloat16)).astype(jnp.float32)
    down = lax.fori_loop(jnp.int32(0), jnp.int32(N_TP), add_group, jnp.zeros((length, down_matrix.shape[1]), jnp.float32))
    return (after_mix + down).astype(jnp.bfloat16)
```

```python
import functools

import jax
import jax.numpy as jnp
from jax import lax
from jax.experimental import pallas as pl
from jax.experimental.pallas import tpu as pltpu
from jax.sharding import PartitionSpec as P

HEAD_WIDTH = 128
EPSILON = 1e-06
PAD = 16
HALO = 8
F32 = jnp.float32
BF16 = jnp.bfloat16
HIGHEST = lax.Precision.HIGHEST
VMEM = 60 * 1024 * 1024


def nt(a, b):
    return lax.dot_general(a, b, (((1,), (1,)), ((), ())), preferred_element_type=F32)


def tn(a, b):
    return lax.dot_general(a, b, (((0,), (0,)), ((), ())), preferred_element_type=F32)


def kernel_call(body, out_shape, *args, flops=10**9):
    n = len(args)
    return pl.pallas_call(
        body,
        out_shape=out_shape,
        in_specs=[pl.BlockSpec(memory_space=pltpu.VMEM)] * n,
        out_specs=jax.tree.map(lambda _: pl.BlockSpec(memory_space=pltpu.VMEM), out_shape),
        compiler_params=pltpu.CompilerParams(vmem_limit_bytes=VMEM),
        cost_estimate=pl.CostEstimate(flops=flops, transcendentals=0, bytes_accessed=10**6),
    )(*args)


def local_body(ff, fb, ql, vw, floor, extra, inside, carry, payload):
    length, width = vw.shape
    heads = width // HEAD_WIDTH
    slices, rows = payload.shape[0], payload.shape[1] - PAD
    per_head = HEAD_WIDTH // rows
    row = lax.broadcasted_iota(jnp.int32, (length, length), 0)
    col = lax.broadcasted_iota(jnp.int32, (length, length), 1)
    seen = (row >= col, row <= col)
    for h in range(heads):
        lanes = slice(h * HEAD_WIDTH, (h + 1) * HEAD_WIDTH)
        q = jax.nn.silu(ql[:, lanes].astype(F32))
        v = vw[:, lanes]
        scores = jnp.zeros((length, length), F32)
        for d, logits in enumerate((ff, fb)):
            z = logits[:, lanes].astype(F32)
            b = floor[d : d + 1, lanes]
            up = jax.nn.sigmoid(z)
            log_forget = jnp.log(b + (1.0 - b) * up) + extra[d, :, h : h + 1]
            key = (1.0 - b) * jax.nn.sigmoid(-z)
            running = jnp.dot(
                seen[d].astype(F32), log_forget, precision=HIGHEST, preferred_element_type=F32
            )
            middle = running[length // 2 : length // 2 + 1]
            total = running[length - 1 : length] if d == 0 else running[0:1]
            rise = jnp.exp(running - middle)
            qd = q * rise
            kd = (key * jnp.exp(middle - running)).astype(BF16)
            scores += jnp.where(seen[d], nt(qd.astype(BF16), kd), 0.0)
            carry[d, :, lanes] = (qd * jnp.exp(middle)).astype(BF16)
            state = (tn(v, kd) * jnp.exp(total - middle)).astype(BF16)
            decay = jnp.exp(total)
            high = decay.astype(BF16)
            low = (decay - high.astype(F32)).astype(BF16)
            tail = jnp.where(
                lax.broadcasted_iota(jnp.int32, (PAD, HEAD_WIDTH), 0) == 0,
                high.astype(F32),
                low.astype(F32),
            ).astype(BF16)
            for i in range(per_head):
                at = (d * heads + h) * per_head + i
                payload[at, 0:rows, :] = state[i * rows : (i + 1) * rows]
                payload[at, rows : rows + PAD, :] = tail
        inside[:, lanes] = jnp.dot(scores.astype(BF16), v, preferred_element_type=F32)


def prefix_body(backward, parts, entering):
    size, rows = entering.shape[0], entering.shape[1]
    flip = backward[0] > 0

    def step(k, state):
        at = jnp.where(flip, size - 1 - k, k)
        entering[at] = state.astype(BF16)
        part = parts[at].astype(F32)
        decay = part[rows : rows + 1] + part[rows + 1 : rows + 2]
        return decay * state + part[0:rows]

    lax.fori_loop(0, size, step, jnp.zeros((rows, HEAD_WIDTH), F32), unroll=True)


def readout_body(inside, carry, entering, gate, scale, gated):
    heads = gated.shape[1] // HEAD_WIDTH
    for h in range(heads):
        lanes = slice(h * HEAD_WIDTH, (h + 1) * HEAD_WIDTH)
        out = inside[:, lanes]
        for d in range(2):
            out = out + nt(carry[d, :, lanes], entering[d, h])
        mean = jnp.mean(out * out, axis=-1, keepdims=True)
        out = out * lax.rsqrt(mean + EPSILON) * scale[...]
        gated[:, lanes] = (out * jax.nn.silu(gate[:, lanes].astype(F32))).astype(BF16)


def convolved(up, taps, own):
    here, before, after = up[0:own], up[own : own + 1], up[own + 1 : own + 2]
    down = jnp.concatenate([before, here[: own - 1]], axis=0)
    ahead = jnp.concatenate([here[1:], after], axis=0)
    return down * taps[0:1] + here * taps[1:2] + ahead * taps[2:3]


def joined(piece):
    return jnp.concatenate([piece[m] for m in range(piece.shape[0])], axis=1)


def up_body(shards, own, n_pieces, x, gate_taps, value_taps, *refs):
    pieces, hidden = refs[:-1], refs[-1]
    width = hidden.shape[2]
    half = x.shape[1] // n_pieces
    ups = []
    for side in range(2):
        total = 0.0
        for p in range(n_pieces):
            total = total + nt(
                x[:, p * half : (p + 1) * half], joined(pieces[side * n_pieces + p])
            )
        ups.append(total.astype(BF16).astype(F32))
    span = own + HALO
    for s in range(shards):
        rows = slice(s * span, (s + 1) * span)
        gate = convolved(ups[0][rows], gate_taps[...], own)
        value = convolved(ups[1][rows], value_taps[...], own)
        hidden[s] = (jax.nn.silu(gate) * value).astype(BF16)


def down_body(hiddens, pieces, *refs):
    hs, ps, out = refs[:hiddens], refs[hiddens : hiddens + pieces * hiddens], refs[-1]
    members = ps[0].shape[0]
    lefts = [h[...] for h in hs]
    for p in range(pieces):
        total = 0.0
        for t in range(hiddens):
            right = joined(ps[t * pieces + p])
            total = total + jnp.dot(lefts[t], right, preferred_element_type=F32)
        out[:, p * members * HEAD_WIDTH : (p + 1) * members * HEAD_WIDTH] = total.astype(BF16)


def on_device(
    residual,
    forget_forward,
    forget_backward,
    value_written,
    query_logits,
    output_gate_logits,
    forget_minimum,
    extra_log_rate,
    head_norm_scale,
    output_matrix,
    prenorm_scale,
    gate_up_matrix,
    value_up_matrix,
    gate_taps,
    value_taps,
    down_matrix,
):
    sp, tp = lax.axis_size("sp"), lax.axis_size("tp")
    s, t = lax.axis_index("sp"), lax.axis_index("tp")
    length, hw = value_written.shape
    heads = hw // HEAD_WIDTH
    own = residual.shape[0]
    model = residual.shape[1]
    lines = sp // 4
    members = lines * 2
    line, side, core = s // 4, (s // 2) % 2, s % 2
    member = line * 2 + core
    columns = [[4 * z + 2 * y + c for z in range(lines) for c in range(2)] for y in range(2)]
    block = model // sp
    width = gate_up_matrix.shape[1] // members

    def swap_side(a):
        return lax.ppermute(a, "sp", [(i, i ^ 2) for i in range(sp)])

    def swap_core(a):
        return lax.ppermute(a, "sp", [(i, i ^ 1) for i in range(sp)])

    def from_line(a, k):
        return lax.ppermute(a, "sp", [(i, (i + 4 * k) % sp) for i in range(sp)])

    def from_rank(a, k):
        return lax.ppermute(a, "tp", [(i, (i + k) % tp) for i in range(tp)])

    rows = 2 * heads * HEAD_WIDTH // sp
    inside, carry, payload = kernel_call(
        local_body,
        (
            jax.ShapeDtypeStruct((length, hw), F32),
            jax.ShapeDtypeStruct((2, length, hw), BF16),
            jax.ShapeDtypeStruct((sp, rows + PAD, HEAD_WIDTH), BF16),
        ),
        forget_forward,
        forget_backward,
        query_logits,
        value_written,
        forget_minimum,
        extra_log_rate,
    )
    parts = lax.all_to_all(payload, "sp", 0, 0, tiled=True)
    backward = (s * rows >= heads * HEAD_WIDTH).astype(jnp.int32).reshape(1)
    prefix = pl.pallas_call(
        prefix_body,
        out_shape=jax.ShapeDtypeStruct((sp, rows, HEAD_WIDTH), BF16),
        in_specs=[
            pl.BlockSpec(memory_space=pltpu.SMEM),
            pl.BlockSpec(memory_space=pltpu.VMEM),
        ],
        out_specs=pl.BlockSpec(memory_space=pltpu.VMEM),
    )(backward, parts)
    entering = lax.all_to_all(prefix, "sp", 0, 0, tiled=True)
    entering = entering.reshape(2, heads, HEAD_WIDTH, HEAD_WIDTH)
    gated = kernel_call(
        readout_body,
        jax.ShapeDtypeStruct((length, hw), BF16),
        inside,
        carry,
        entering,
        output_gate_logits,
        head_norm_scale.reshape(1, HEAD_WIDTH),
    )

    out_rows = lax.dynamic_slice_in_dim(output_matrix, t * hw, hw, 0)
    out_own = lax.all_gather(
        out_rows, "sp", axis_index_groups=columns, axis=0
    )
    out_both = jnp.stack([out_own, swap_side(out_own)])

    def by_side(a, axis):
        shape = a.shape[:axis] + (lines, 2, 2, block) + a.shape[axis + 1 :]
        a = jnp.moveaxis(a.reshape(shape), axis + 1, axis)
        first = lax.dynamic_index_in_dim(a, side, axis, keepdims=True)
        second = lax.dynamic_index_in_dim(a, 1 - side, axis, keepdims=True)
        return jnp.concatenate([first, second], axis).reshape(
            a.shape[:axis] + (model,) + a.shape[axis + 4 :]
        )

    part = jnp.einsum("tk,ymkn->tymn", gated, out_both, preferred_element_type=F32)
    part = part.reshape(length, model)
    mixed = lax.dynamic_slice_in_dim(part, t * own, own, 0)
    for k in range(1, tp):
        to = (t + k) % tp
        sent = lax.dynamic_slice_in_dim(part, to * own, own, 0).astype(BF16)
        mixed = mixed + from_rank(sent, k).astype(F32)
    after = by_side(residual, 1).astype(F32) + mixed
    scale = lax.rsqrt(jnp.mean(after * after, axis=-1, keepdims=True) + EPSILON)
    normed = (after * scale * by_side(prenorm_scale, 0)).astype(BF16)

    count = sp * tp
    ahead = [(i, i + 1) for i in range(count - 1)]
    behind = [(i + 1, i) for i in range(count - 1)]
    def natural(a):
        a = a.reshape(a.shape[0], 2, lines, 2, block)
        low = lax.dynamic_index_in_dim(a, side, 1, keepdims=True)
        high = lax.dynamic_index_in_dim(a, 1 - side, 1, keepdims=True)
        return jnp.moveaxis(jnp.concatenate([low, high], 1), 1, 2).reshape(a.shape[0], model)

    edges = natural(jnp.concatenate([normed[:1], normed[own - 1 :]], 0))
    before = lax.ppermute(edges[1:2], ("sp", "tp"), ahead)
    following = lax.ppermute(edges[0:1], ("sp", "tp"), behind)
    halo = by_side(jnp.concatenate([before, following], 0), 1)
    halo = jnp.pad(halo, ((0, HALO - 2), (0, 0)))
    shard = jnp.concatenate([normed, halo], 0)
    shards = [shard] + [from_line(shard, k) for k in range(1, lines)]
    tokens = jnp.concatenate(shards, 0)
    tokens = jnp.concatenate([tokens, swap_core(tokens)], 0)

    def spread(piece):
        got = lax.all_to_all(piece, "sp", 0, 0, axis_index_groups=columns, tiled=True)
        pieces = [(got, swap_side(got))]
        cut = members // 2
        for k in range(1, tp):
            rank = from_rank(got, k)
            low = swap_side(rank[:cut])
            high = from_rank(pieces[0][1][cut:], k)
            pieces.append((rank, jnp.concatenate([low, high], 0)))
        return pieces

    gates = spread(gate_up_matrix.T.reshape(members, width, block))
    values = spread(value_up_matrix.T.reshape(members, width, block))
    downs = spread(down_matrix.reshape(members, width, block))
    taps = jnp.concatenate([gate_taps, value_taps], 0)
    taps = lax.dynamic_slice_in_dim(taps, member * width, width, 1)
    taps = [taps] + [from_rank(taps, k) for k in range(1, tp)]

    plain = block == HEAD_WIDTH
    hiddens = []
    for k in range(tp):
        if plain:
            hidden = kernel_call(
                functools.partial(up_body, members, own, 2),
                jax.ShapeDtypeStruct((members, own, width), BF16),
                tokens,
                taps[k][:3],
                taps[k][3:],
                *gates[k],
                *values[k],
            ).reshape(members * own, width)
        else:
            x = tokens.reshape(-1, 2, members, block)
            up = [
                jnp.einsum("nymd,ymhd->nh", x, jnp.stack(w[k]), preferred_element_type=F32)
                .astype(BF16)
                .reshape(members, own + HALO, width)
                for w in (gates, values)
            ]
            conv = jax.vmap(convolved, (0, None, None))
            hidden = (jax.nn.silu(conv(up[0], taps[k][:3], own)) * conv(up[1], taps[k][3:], own))
            hidden = hidden.astype(BF16).reshape(members * own, width)
        hiddens.append(hidden)
    if plain:
        terms = kernel_call(
            functools.partial(down_body, tp, 2),
            jax.ShapeDtypeStruct((members * own, model), BF16),
            *hiddens,
            *[p for k in range(tp) for p in downs[k]],
        )
    else:
        terms = sum(
            jnp.einsum("nh,ymhd->nymd", hiddens[k], jnp.stack(downs[k]), preferred_element_type=F32)
            for k in range(tp)
        )
        terms = terms.astype(BF16).reshape(members * own, model)

    half = lines * own
    terms = terms[:half].astype(F32) + swap_core(terms[half:]).astype(F32)
    total = after + terms[:own]
    for k in range(1, lines):
        sent = terms[k * own : (k + 1) * own].astype(BF16)
        total = total + from_line(sent, lines - k).astype(F32)
    return natural(total).astype(BF16)


def solution(mesh):
    return jax.shard_map(
        on_device,
        mesh=mesh,
        in_specs=(
            P(("sp", "tp"), None),
            P("sp", "tp"),
            P("sp", "tp"),
            P("sp", "tp"),
            P("sp", "tp"),
            P("sp", "tp"),
            P(None, "tp"),
            P(None, "sp", "tp"),
            P(),
            P(None, "sp"),
            P(),
            P("sp", "tp"),
            P("sp", "tp"),
            P(None, "tp"),
            P(None, "tp"),
            P("tp", "sp"),
        ),
        out_specs=P(("sp", "tp"), None),
        check_vma=False,
    )
```
